32 devices in a mesh: fs: 8 (over z, y), tp: 4 (over x, core).
Axes of the slice: x: 2, y: 2, z: 4, core: 2. Of those that a mesh axis runs over, the one named last changes fastest.
Arguments:
- inputs: bfloat16 [24576, 2048], P('fs'), may hold values from -6 to 6
- cot_query: bfloat16 [24576, 2048], P('fs', 'tp'), may hold values from -0.09375 to 0.09375
- cot_value: bfloat16 [24576, 4096], P('fs', 'tp'), may hold values from -0.09375 to 0.09375
- proj_query: bfloat16 [2048, 256], replicated, may hold values from -0.375 to 0.375
- proj_value: bfloat16 [2048, 256], replicated, may hold values from -0.375 to 0.375
- w_query: float32 [2048, 2048], P('fs', 'tp'), may hold values from -6 to 6
- w_value: float32 [2048, 4096], P('fs', 'tp'), may hold values from -6 to 6
- m_query: float32 [256, 2048], P('fs', 'tp'), may hold values from -30 to 30
- m_value: float32 [256, 4096], P('fs', 'tp'), may hold values from -30 to 30
- v_query: float32 [256, 2048], P('fs', 'tp'), may hold values from 0.05 to 2
- v_value: float32 [256, 4096], P('fs', 'tp'), may hold values from 0.05 to 2
Outputs:
- new_query: float32 [2048, 2048], P('fs', 'tp')
- new_value: float32 [2048, 4096], P('fs', 'tp')
- copy_query: bfloat16 [2048, 2048], P(None, 'tp')
- copy_value: bfloat16 [2048, 4096], P(None, 'tp')
- first_query: float32 [256, 2048], P('fs', 'tp')
- first_value: float32 [256, 4096], P('fs', 'tp')
- second_query: float32 [256, 2048], P('fs', 'tp')
- second_value: float32 [256, 4096], P('fs', 'tp')
- step_query: float32 [2048, 2048], P('fs', 'tp')
- step_value: float32 [2048, 4096], P('fs', 'tp')
The draws below stay inside these ranges and needn't reach their ends.
All inputs are finite; a program needn't handle non-finite values.
Results may differ from the reference program's by a relative error of at most 0.015.
Values may be sent and summed in bfloat16 or wider, within the bound.
A program may use at most 128 MiB of HBM per device.

```python
import math
import jax
import jax.numpy as jnp
from jax import lax

D = 2048
RANK = 256
QK_W = 2048
V_W = 4096
TOKENS = 24576


def moment_draw(key, rows, cols):
    base = jax.random.normal(jax.random.fold_in(key, 11), (rows, cols), jnp.float32)
    base = jnp.clip(base, -5.0, 5.0) * 0.5
    row_scale = (4.0 ** (jnp.arange(rows, dtype=jnp.float32) / rows))[:, None]
    col_scale = (3.0 ** (jnp.arange(cols, dtype=jnp.float32) / cols))[None, :]
    return base * row_scale * col_scale


def draw_m_query(key, part):
    return moment_draw(key, RANK, QK_W)


def draw_m_value(key, part):
    return moment_draw(key, RANK, V_W)


def levels(stream_key, shape, pieces, low, high):
    def one(axis_at, parts):
        draws = jax.random.uniform(jax.random.fold_in(jax.random.fold_in(stream_key, 6), axis_at), (parts,), jnp.float32, low / len(pieces), high / len(pieces))
        return jnp.repeat(jnp.exp(draws), shape[axis_at] // parts).reshape((-1,) + (1,) * (len(shape) - axis_at - 1))

    loudness = one(*pieces[0])
    for cut in pieces[1:]:
        loudness = loudness * one(*cut)
    return loudness


def normal_values(own_key, extent, scale, limit, cuts=(), held_as=jnp.bfloat16):
    loudness = levels(own_key, extent, cuts, -0.22, 0.18) if cuts else 1.0
    drawn = jax.random.normal(own_key, extent, jnp.float32) * scale * loudness
    return jnp.minimum(jnp.maximum(drawn, -limit), limit).astype(held_as)


def setup_inputs(seed: int = 0) -> dict:
    splits = jax.random.split(jax.random.key(seed), 12)
    return {
        "inputs": normal_values(splits[0], (TOKENS, D), 1.0, 6.0, ((0, 8),)),
        "cot_query": normal_values(splits[1], (TOKENS, QK_W), (TOKENS ** -0.5), 0.09375, ((0, 8), (1, 4))),
        "cot_value": normal_values(splits[2], (TOKENS, V_W), (TOKENS ** -0.5), 0.09375, ((0, 8), (1, 4))),
        "proj_query": normal_values(splits[3], (D, RANK), RANK ** -0.5, 0.375),
        "proj_value": normal_values(splits[4], (D, RANK), RANK ** -0.5, 0.375),
        "w_query": normal_values(splits[5], (D, QK_W), 1.0, 6.0, ((0, 8), (1, 4)), jnp.float32),
        "w_value": normal_values(splits[6], (D, V_W), 1.0, 6.0, ((0, 8), (1, 4)), jnp.float32),
        "m_query": draw_m_query(jax.random.fold_in(splits[11], 71), 0),
        "m_value": draw_m_value(jax.random.fold_in(splits[11], 71), 0),
        "v_query": jnp.clip(jnp.exp(math.log(2.0) - 3.6888794 * jax.random.uniform(splits[9], (RANK, QK_W), jnp.float32) ** levels(splits[9], (RANK, QK_W), ((0, 8), (1, 4)), -0.2, 0.2)), 0.05, 2.0),
        "v_value": jnp.clip(jnp.exp(math.log(2.0) - 3.6888794 * jax.random.uniform(splits[10], (RANK, V_W), jnp.float32) ** levels(splits[10], (RANK, V_W), ((0, 8), (1, 4)), -0.2, 0.2)), 0.05, 2.0),
    }


beta_first = 0.9
beta_second = 0.95
adam_eps = 1e-08
norm_eps = 1e-06
step_rate = 0.05
decay_rate = 0.2

def moment_update(factor, gradient, first, second):
    low = jnp.dot(factor.astype(jnp.float32).T, gradient, precision=lax.Precision.HIGHEST)
    first_new = beta_first * first + (1.0 - beta_first) * low
    second_new = beta_second * second + (1.0 - beta_second) * low * low
    update = first_new / (jnp.sqrt(second_new) + adam_eps)
    return (first_new, second_new, update)

def reference(inputs, cot_query, cot_value, proj_query, proj_value, w_query, w_value, m_query, m_value, v_query, v_value):
    grad_query = jnp.dot(inputs.T, cot_query, preferred_element_type=jnp.float32)
    grad_value = jnp.dot(inputs.T, cot_value, preferred_element_type=jnp.float32)
    first_query, second_query, update_query = moment_update(proj_query, grad_query, m_query, v_query)
    first_value, second_value, update_value = moment_update(proj_value, grad_value, m_value, v_value)
    total = jnp.sum(update_query * update_query) + jnp.sum(update_value * update_value)
    scale = lax.rsqrt(total / (RANK * (QK_W + V_W)) + norm_eps)
    step_query = scale * jnp.dot(proj_query.astype(jnp.float32), update_query, precision=lax.Precision.HIGHEST) + decay_rate * w_query
    step_value = scale * jnp.dot(proj_value.astype(jnp.float32), update_value, precision=lax.Precision.HIGHEST) + decay_rate * w_value
    new_query = w_query - step_rate * step_query
    new_value = w_value - step_rate * step_value
    return (new_query, new_value, new_query.astype(jnp.bfloat16), new_value.astype(jnp.bfloat16), first_query, first_value, second_query, second_value, step_query, step_value)
```

```python
import functools

import jax
import jax.numpy as jnp
from jax import lax
from jax.experimental import pallas as pl
from jax.experimental.pallas import tpu as pltpu
from jax.sharding import PartitionSpec as P

beta_first = 0.9
beta_second = 0.95
adam_eps = 1e-08
norm_eps = 1e-06
step_rate = 0.05
decay_rate = 0.2


def moments(low, first, second):
    first_new = beta_first * first + (1.0 - beta_first) * low
    second_new = beta_second * second + (1.0 - beta_second) * low * low
    return first_new, second_new


def update_of(low, first, second):
    first_new, second_new = moments(low, first, second)
    return first_new / (jnp.sqrt(second_new) + adam_eps)


def ring_order(n):
    if n % 4 or n < 8:
        return list(range(n))
    cols = n // 4
    cycle = [0]
    for z in range(4):
        span = range(1, cols) if z % 2 == 0 else range(cols - 1, 0, -1)
        cycle += [z * cols + y for y in span]
    return cycle + [z * cols for z in (3, 2, 1)]


def lookup(table, index):
    value = jnp.int32(table[0])
    for k in range(1, len(table)):
        value = jnp.where(index == k, jnp.int32(table[k]), value)
    return value


def kernel(
    n,
    t,
    tile,
    x_hbm,
    cq_hbm,
    cv_hbm,
    pq_ref,
    pv_ref,
    wq_ref,
    wv_ref,
    mq_ref,
    mv_ref,
    vq_ref,
    vv_ref,
    gq_hbm,
    gv_hbm,
    uq_ref,
    uv_ref,
    lowq_ref,
    lowv_ref,
    total_ref,
    acc_q,
    acc_v,
    part_q,
    part_v,
    got_q,
    got_v,
    sums,
    w_send,
    w_recv,
    own_sem,
    r_send,
    r_recv,
    u_send,
    u_recv,
    t_send,
    t_recv,
):
    me = lax.axis_index("fs")
    col = lax.axis_index("tp")
    order = ring_order(n)
    place = [order.index(k) for k in range(n)]
    pos = lookup(place, me)

    def at(step):
        return lookup(order, lax.rem(pos + step + 2 * n, n))

    rows = wq_ref.shape[0]
    half_rows = rows // 2
    ranks = mq_ref.shape[0]

    barrier = pltpu.get_barrier_semaphore()
    for d in range(1, n):
        pl.semaphore_signal(
            barrier, inc=1, device_id={"fs": lax.rem(me + d, n)}, device_id_type=pl.DeviceIdType.MESH
        )
    for d in range(1, t):
        pl.semaphore_signal(
            barrier, inc=1, device_id={"tp": lax.rem(col + d, t)}, device_id_type=pl.DeviceIdType.MESH
        )
    pl.semaphore_wait(barrier, n - 1 + t - 1)

    def reach(way, half):
        return n // 2 if way == half else n - 1 - n // 2

    sign = (1, -1)

    def w_copy(way, half, hop):
        owner = at(-sign[way] * hop)
        target = at(sign[way])
        copies = []
        for k, (own, out) in enumerate(((wq_ref, gq_hbm), (wv_ref, gv_hbm))):
            place_ = pl.ds(pl.multiple_of(owner * rows + half * half_rows, half_rows), half_rows)
            src = own.at[pl.ds(half * half_rows, half_rows)] if hop == 0 else out.at[place_]
            copies.append(
                pltpu.make_async_remote_copy(
                    src_ref=src,
                    dst_ref=out.at[place_],
                    send_sem=w_send.at[way, half, hop, k],
                    recv_sem=w_recv.at[way, half, hop, k],
                    device_id={"fs": target},
                    device_id_type=pl.DeviceIdType.MESH,
                )
            )
        return copies

    def w_arrived(way, half, hop):
        owner = at(-sign[way] * (hop + 1))
        for k, out in enumerate((gq_hbm, gv_hbm)):
            place_ = pl.ds(pl.multiple_of(owner * rows + half * half_rows, half_rows), half_rows)
            pltpu.make_async_remote_copy(
                src_ref=out.at[place_],
                dst_ref=out.at[place_],
                send_sem=w_send.at[way, half, hop, k],
                recv_sem=w_recv.at[way, half, hop, k],
                device_id={"fs": at(sign[way])},
                device_id_type=pl.DeviceIdType.MESH,
            ).wait_recv()

    started = []

    def send_w(hop):
        for half in range(2):
            for way in range(2):
                if hop and hop - 1 < reach(way, half):
                    w_arrived(way, half, hop - 1)
                if hop < reach(way, half):
                    for copy in w_copy(way, half, hop):
                        copy.start()
                        started.append(copy)

    send_w(0)
    mine = pl.ds(pl.multiple_of(me * rows, rows), rows)
    own = [
        pltpu.make_async_copy(wq_ref, gq_hbm.at[mine], own_sem.at[0]),
        pltpu.make_async_copy(wv_ref, gv_hbm.at[mine], own_sem.at[1]),
    ]
    for copy in own:
        copy.start()

    acc_q[...] = jnp.zeros_like(acc_q)
    acc_v[...] = jnp.zeros_like(acc_v)

    def lead(left, right):
        return lax.dot_general(
            left, right, (((0,), (0,)), ((), ())), preferred_element_type=jnp.float32
        )

    def body(x, cq, cv):
        values = x[...]
        mixed_q = jnp.dot(values, pq_ref[...], preferred_element_type=jnp.float32)
        acc_q[...] += lead(mixed_q.astype(jnp.bfloat16), cq[...])
        mixed_v = jnp.dot(values, pv_ref[...], preferred_element_type=jnp.float32)
        acc_v[...] += lead(mixed_v.astype(jnp.bfloat16), cv[...])

    pltpu.emit_pipeline(
        body,
        grid=(x_hbm.shape[0] // tile,),
        in_specs=[
            pl.BlockSpec((tile, x_hbm.shape[1]), lambda i: (i, 0)),
            pl.BlockSpec((tile, cq_hbm.shape[1]), lambda i: (i, 0)),
            pl.BlockSpec((tile, cv_hbm.shape[1]), lambda i: (i, 0)),
        ],
        out_specs=[],
    )(x_hbm, cq_hbm, cv_hbm)

    part_q[...] = acc_q[...].astype(jnp.bfloat16)
    part_v[...] = acc_v[...].astype(jnp.bfloat16)
    scattered = []
    for d in range(1, n):
        target = lax.rem(me + d, n)
        chunk = pl.ds(pl.multiple_of(target * ranks, ranks), ranks)
        for k, (part, got) in enumerate(((part_q, got_q), (part_v, got_v))):
            copy = pltpu.make_async_remote_copy(
                src_ref=part.at[chunk],
                dst_ref=got.at[d - 1],
                send_sem=r_send.at[d - 1, k],
                recv_sem=r_recv.at[d - 1, k],
                device_id={"fs": target},
                device_id_type=pl.DeviceIdType.MESH,
            )
            copy.start()
            scattered.append(copy)

    send_w(1)

    for copy in scattered:
        copy.wait_recv()
    kept = pl.ds(pl.multiple_of(me * ranks, ranks), ranks)
    for acc, got, low_ref, m_ref, v_ref, u_ref in (
        (acc_q, got_q, lowq_ref, mq_ref, vq_ref, uq_ref),
        (acc_v, got_v, lowv_ref, mv_ref, vv_ref, uv_ref),
    ):
        low = acc[kept, :]
        for d in range(n - 1):
            low = low + got[d].astype(jnp.float32)
        low_ref[...] = low
        u_ref[kept, :] = update_of(low, m_ref[...], v_ref[...]).astype(jnp.bfloat16)

    gathered = []
    for d in range(1, n):
        for k, u_ref in enumerate((uq_ref, uv_ref)):
            copy = pltpu.make_async_remote_copy(
                src_ref=u_ref.at[kept],
                dst_ref=u_ref.at[kept],
                send_sem=u_send.at[d - 1, k],
                recv_sem=u_recv.at[d - 1, k],
                device_id={"fs": lax.rem(me + d, n)},
                device_id_type=pl.DeviceIdType.MESH,
            )
            copy.start()
            gathered.append(copy)

    send_w(2)

    for d in range(1, n):
        source = lax.rem(me - d + n, n)
        chunk = pl.ds(pl.multiple_of(source * ranks, ranks), ranks)
        for k, u_ref in enumerate((uq_ref, uv_ref)):
            pltpu.make_async_remote_copy(
                src_ref=u_ref.at[chunk],
                dst_ref=u_ref.at[chunk],
                send_sem=u_send.at[d - 1, k],
                recv_sem=u_recv.at[d - 1, k],
                device_id={"fs": source},
                device_id_type=pl.DeviceIdType.MESH,
            ).wait_recv()

    square = jnp.float32(0)
    for u_ref in (uq_ref, uv_ref):
        values = u_ref[...].astype(jnp.float32)
        square = square + jnp.sum(values * values)
    sums[0] = jnp.full(sums.shape[1:], square, jnp.float32)
    shared = []
    for d in range(1, t):
        copy = pltpu.make_async_remote_copy(
            src_ref=sums.at[0],
            dst_ref=sums.at[d],
            send_sem=t_send.at[d - 1],
            recv_sem=t_recv.at[d - 1],
            device_id={"tp": lax.rem(col + d, t)},
            device_id_type=pl.DeviceIdType.MESH,
        )
        copy.start()
        shared.append(copy)

    for hop in range(3, n // 2 + 1):
        send_w(hop)

    for copy in shared:
        copy.wait_recv()
    total_ref[...] = jnp.sum(sums[...], axis=0)
    for copy in own:
        copy.wait()
    for copy in started + scattered + gathered + shared:
        copy.wait_send()


def on_device(n, t, inputs, cot_query, cot_value, proj_query, proj_value,
              w_query, w_value, m_query, m_value, v_query, v_value):
    depth = proj_query.shape[0]
    rank = proj_query.shape[1]
    ranks = m_query.shape[0]
    rows = w_query.shape[0]
    width_q = w_query.shape[1]
    width_v = w_value.shape[1]
    tokens = inputs.shape[0]
    tile = 512 if tokens % 512 == 0 else tokens
    half = jnp.bfloat16
    full = jnp.float32
    anywhere = pl.BlockSpec(memory_space=pl.ANY)
    inside = pl.BlockSpec(memory_space=pltpu.VMEM)
    hops = n // 2
    gq, gv, uq, uv, lowq, lowv, total = pl.pallas_call(
        functools.partial(kernel, n, t, tile),
        out_shape=(
            jax.ShapeDtypeStruct((depth, width_q), half),
            jax.ShapeDtypeStruct((depth, width_v), half),
            jax.ShapeDtypeStruct((rank, width_q), half),
            jax.ShapeDtypeStruct((rank, width_v), half),
            jax.ShapeDtypeStruct((ranks, width_q), full),
            jax.ShapeDtypeStruct((ranks, width_v), full),
            jax.ShapeDtypeStruct((8, 128), full),
        ),
        in_specs=[anywhere] * 3 + [inside] * 8,
        out_specs=(anywhere,) * 2 + (inside,) * 5,
        scratch_shapes=[
            pltpu.VMEM((rank, width_q), full),
            pltpu.VMEM((rank, width_v), full),
            pltpu.VMEM((rank, width_q), half),
            pltpu.VMEM((rank, width_v), half),
            pltpu.VMEM((n - 1, ranks, width_q), half),
            pltpu.VMEM((n - 1, ranks, width_v), half),
            pltpu.VMEM((t, 8, 128), full),
            pltpu.SemaphoreType.DMA((2, 2, hops, 2)),
            pltpu.SemaphoreType.DMA((2, 2, hops, 2)),
            pltpu.SemaphoreType.DMA((2,)),
            pltpu.SemaphoreType.DMA((n - 1, 2)),
            pltpu.SemaphoreType.DMA((n - 1, 2)),
            pltpu.SemaphoreType.DMA((n - 1, 2)),
            pltpu.SemaphoreType.DMA((n - 1, 2)),
            pltpu.SemaphoreType.DMA((t - 1,)),
            pltpu.SemaphoreType.DMA((t - 1,)),
        ],
        compiler_params=pltpu.CompilerParams(
            collective_id=0, has_side_effects=True, vmem_limit_bytes=48 * 2**20
        ),
    )(
        inputs, cot_query, cot_value, proj_query, proj_value,
        w_query.astype(half), w_value.astype(half),
        m_query, m_value, v_query, v_value,
    )
    first_query, second_query = moments(lowq, m_query, v_query)
    first_value, second_value = moments(lowv, m_value, v_value)
    count = rank * t * (width_q + width_v)
    scale = lax.rsqrt(total[0, 0] / count + norm_eps)
    offset = lax.axis_index("fs") * rows
    local_q = lax.dynamic_slice_in_dim(proj_query, offset, rows, 0)
    local_v = lax.dynamic_slice_in_dim(proj_value, offset, rows, 0)

    def dot(a, b):
        return jnp.dot(a, b, preferred_element_type=full)

    def whole(kept, factor, update):
        step = scale * dot(factor, update) + decay_rate * kept.astype(full)
        return (kept.astype(full) - step_rate * step).astype(half)

    step_query = scale * dot(local_q, uq) + decay_rate * w_query
    step_value = scale * dot(local_v, uv) + decay_rate * w_value
    new_query = w_query - step_rate * step_query
    new_value = w_value - step_rate * step_value
    return (
        new_query,
        new_value,
        whole(gq, proj_query, uq),
        whole(gv, proj_value, uv),
        first_query,
        first_value,
        second_query,
        second_value,
        step_query,
        step_value,
    )


def solution(mesh):
    n = mesh.shape["fs"]
    t = mesh.shape["tp"]
    split = P("fs", "tp")
    return jax.shard_map(
        functools.partial(on_device, n, t),
        mesh=mesh,
        in_specs=(P("fs", None), split, split, P(), P()) + (split,) * 6,
        out_specs=(split, split, P(None, "tp"), P(None, "tp")) + (split,) * 6,
        check_vma=False,
    )
```

```python
import functools

import jax
import jax.numpy as jnp
from jax import lax
from jax.experimental import pallas as pl
from jax.experimental.pallas import tpu as pltpu
from jax.sharding import PartitionSpec as P

beta_first = 0.9
beta_second = 0.95
adam_eps = 1e-08
norm_eps = 1e-06
step_rate = 0.05
decay_rate = 0.2


def moments(low, first, second):
    first_new = beta_first * first + (1.0 - beta_first) * low
    second_new = beta_second * second + (1.0 - beta_second) * low * low
    return first_new, second_new


def update_of(low, first, second):
    first_new, second_new = moments(low, first, second)
    return first_new / (jnp.sqrt(second_new) + adam_eps)


def ring_order(n):
    if n % 4 or n < 8:
        return list(range(n))
    cols = n // 4
    cycle = [0]
    for z in range(4):
        span = range(1, cols) if z % 2 == 0 else range(cols - 1, 0, -1)
        cycle += [z * cols + y for y in span]
    return cycle + [z * cols for z in (3, 2, 1)]


def lookup(table, index):
    value = jnp.int32(table[0])
    for k in range(1, len(table)):
        value = jnp.where(index == k, jnp.int32(table[k]), value)
    return value


def kernel(
    n,
    t,
    tile,
    x_hbm,
    cq_hbm,
    cv_hbm,
    pq_hbm,
    pv_hbm,
    wq_ref,
    wv_ref,
    mq_hbm,
    mv_hbm,
    vq_hbm,
    vv_hbm,
    gq_hbm,
    gv_hbm,
    uq_ref,
    uv_ref,
    lowq_ref,
    lowv_ref,
    total_ref,
    acc_q,
    acc_v,
    part_q,
    part_v,
    near_q,
    near_v,
    got_q,
    got_v,
    sums,
    pq_ref,
    pv_ref,
    mq_ref,
    mv_ref,
    vq_ref,
    vv_ref,
    load_sem,
    y_send,
    y_recv,
    f_send,
    f_recv,
    w_send,
    w_recv,
    own_sem,
    r_send,
    r_recv,
    u_send,
    u_recv,
    t_send,
    t_recv,
):
    me = lax.axis_index("fs")
    col = lax.axis_index("tp")
    order = ring_order(n)
    place = [order.index(k) for k in range(n)]
    pos = lookup(place, me)

    def at(step):
        return lookup(order, lax.rem(pos + step + 2 * n, n))

    rows = wq_ref.shape[0]
    half_rows = rows // 2
    ranks = mq_ref.shape[0]

    barrier = pltpu.get_barrier_semaphore()
    for d in range(1, n):
        pl.semaphore_signal(
            barrier, inc=1, device_id={"fs": lax.rem(me + d, n)}, device_id_type=pl.DeviceIdType.MESH
        )
    for d in range(1, t):
        pl.semaphore_signal(
            barrier, inc=1, device_id={"tp": lax.rem(col + d, t)}, device_id_type=pl.DeviceIdType.MESH
        )
    pl.semaphore_wait(barrier, n - 1 + t - 1)

    def reach(way, half):
        return n // 2 if way == half else n - 1 - n // 2

    sign = (1, -1)

    def w_copy(way, half, hop):
        owner = at(-sign[way] * hop)
        target = at(sign[way])
        copies = []
        for k, (own, out) in enumerate(((wq_ref, gq_hbm), (wv_ref, gv_hbm))):
            place_ = pl.ds(pl.multiple_of(owner * rows + half * half_rows, half_rows), half_rows)
            src = own.at[pl.ds(half * half_rows, half_rows)] if hop == 0 else out.at[place_]
            copies.append(
                pltpu.make_async_remote_copy(
                    src_ref=src,
                    dst_ref=out.at[place_],
                    send_sem=w_send.at[way, half, hop, k],
                    recv_sem=w_recv.at[way, half, hop, k],
                    device_id={"fs": target},
                    device_id_type=pl.DeviceIdType.MESH,
                )
            )
        return copies

    def w_arrived(way, half, hop):
        owner = at(-sign[way] * (hop + 1))
        for k, out in enumerate((gq_hbm, gv_hbm)):
            place_ = pl.ds(pl.multiple_of(owner * rows + half * half_rows, half_rows), half_rows)
            pltpu.make_async_remote_copy(
                src_ref=out.at[place_],
                dst_ref=out.at[place_],
                send_sem=w_send.at[way, half, hop, k],
                recv_sem=w_recv.at[way, half, hop, k],
                device_id={"fs": at(sign[way])},
                device_id_type=pl.DeviceIdType.MESH,
            ).wait_recv()

    started = []

    def send_w(hop, halves=(0, 1)):
        for half in halves:
            for way in range(2):
                if hop and hop - 1 < reach(way, half):
                    w_arrived(way, half, hop - 1)
                if hop < reach(way, half):
                    for copy in w_copy(way, half, hop):
                        copy.start()
                        started.append(copy)

    send_w(0)
    mine = pl.ds(pl.multiple_of(me * rows, rows), rows)
    own = [
        pltpu.make_async_copy(wq_ref, gq_hbm.at[mine], own_sem.at[0]),
        pltpu.make_async_copy(wv_ref, gv_hbm.at[mine], own_sem.at[1]),
    ]
    loads = [
        pltpu.make_async_copy(src, dst, load_sem.at[k])
        for k, (src, dst) in enumerate(
            (
                (pq_hbm, pq_ref),
                (pv_hbm, pv_ref),
                (mq_hbm, mq_ref),
                (mv_hbm, mv_ref),
                (vq_hbm, vq_ref),
                (vv_hbm, vv_ref),
            )
        )
    ]
    for copy in loads + own:
        copy.start()

    acc_q[...] = jnp.zeros_like(acc_q)
    acc_v[...] = jnp.zeros_like(acc_v)

    for copy in loads:
        copy.wait()

    def lead(left, right):
        return lax.dot_general(
            left, right, (((0,), (0,)), ((), ())), preferred_element_type=jnp.float32
        )

    def body(x, cq, cv):
        values = x[...]
        mixed_q = jnp.dot(values, pq_ref[...], preferred_element_type=jnp.float32)
        acc_q[...] += lead(mixed_q.astype(jnp.bfloat16), cq[...])
        mixed_v = jnp.dot(values, pv_ref[...], preferred_element_type=jnp.float32)
        acc_v[...] += lead(mixed_v.astype(jnp.bfloat16), cv[...])

    pltpu.emit_pipeline(
        body,
        grid=(x_hbm.shape[0] // tile,),
        in_specs=[
            pl.BlockSpec((tile, x_hbm.shape[1]), lambda i: (i, 0)),
            pl.BlockSpec((tile, cq_hbm.shape[1]), lambda i: (i, 0)),
            pl.BlockSpec((tile, cv_hbm.shape[1]), lambda i: (i, 0)),
        ],
        out_specs=[],
    )(x_hbm, cq_hbm, cv_hbm)

    zs, ys = part_q.shape[:2]
    my_z, my_y = me // ys, lax.rem(me, ys)
    pairs = ((acc_q, part_q, near_q, got_q), (acc_v, part_v, near_v, got_v))

    def remote(src, dst, send, recv, target):
        return pltpu.make_async_remote_copy(
            src_ref=src,
            dst_ref=dst,
            send_sem=send,
            recv_sem=recv,
            device_id={"fs": target},
            device_id_type=pl.DeviceIdType.MESH,
        )

    for acc, part, near, got in pairs:
        for z in range(zs):
            for y in range(ys):
                start = (z * ys + y) * ranks
                part[z, y] = acc[start : start + ranks, :].astype(jnp.bfloat16)
    across = []
    for d in range(1, ys):
        other = lax.rem(my_y + d, ys)
        for k, (acc, part, near, got) in enumerate(pairs):
            copy = remote(
                part.at[:, other],
                near.at[d - 1],
                y_send.at[d - 1, k],
                y_recv.at[d - 1, k],
                my_z * ys + other,
            )
            copy.start()
            across.append(copy)

    send_w(1, (0,))

    for copy in across:
        copy.wait_recv()
    for acc, part, near, got in pairs:
        for z in range(zs):
            start = pl.multiple_of((z * ys + my_y) * ranks, ranks)
            value = acc[pl.ds(start, ranks), :]
            for d in range(ys - 1):
                value = value + near[d, z].astype(jnp.float32)
            acc[pl.ds(start, ranks), :] = value
            near[ys - 1, z] = value.astype(jnp.bfloat16)
    along = []
    for d in range(1, zs):
        other = lax.rem(my_z + d, zs)
        for k, (acc, part, near, got) in enumerate(pairs):
            copy = remote(
                near.at[ys - 1, other],
                got.at[d - 1],
                r_send.at[d - 1, k],
                r_recv.at[d - 1, k],
                other * ys + my_y,
            )
            copy.start()
            along.append(copy)

    send_w(1, (1,))

    for copy in along:
        copy.wait_recv()
    kept = pl.ds(pl.multiple_of(me * ranks, ranks), ranks)
    for acc, got, low_ref, m_ref, v_ref, u_ref in (
        (acc_q, got_q, lowq_ref, mq_ref, vq_ref, uq_ref),
        (acc_v, got_v, lowv_ref, mv_ref, vv_ref, uv_ref),
    ):
        low = acc[kept, :]
        for d in range(zs - 1):
            low = low + got[d].astype(jnp.float32)
        low_ref[...] = low
        u_ref[kept, :] = update_of(low, m_ref[...], v_ref[...]).astype(jnp.bfloat16)

    def block(z, y):
        return pl.ds(pl.multiple_of((z * ys + y) * ranks, ranks), ranks)

    gathered = []
    for d in range(1, zs):
        for k, u_ref in enumerate((uq_ref, uv_ref)):
            copy = remote(
                u_ref.at[kept],
                u_ref.at[kept],
                u_send.at[d - 1, k],
                u_recv.at[d - 1, k],
                lax.rem(my_z + d, zs) * ys + my_y,
            )
            copy.start()
            gathered.append(copy)

    def forward(z, s):
        for d in range(1, ys):
            for k, u_ref in enumerate((uq_ref, uv_ref)):
                copy = remote(
                    u_ref.at[block(z, my_y)],
                    u_ref.at[block(z, my_y)],
                    f_send.at[d - 1, s, k],
                    f_recv.at[d - 1, s, k],
                    my_z * ys + lax.rem(my_y + d, ys),
                )
                copy.start()
                gathered.append(copy)

    forward(my_z, 0)

    send_w(2, (0,))

    for d in range(1, zs):
        source = lax.rem(my_z - d + zs, zs)
        for k, u_ref in enumerate((uq_ref, uv_ref)):
            rows_ = u_ref.at[block(source, my_y)]
            remote(
                rows_, rows_, u_send.at[d - 1, k], u_recv.at[d - 1, k], source * ys + my_y
            ).wait_recv()
        forward(source, d)

    send_w(2, (1,))

    for d in range(1, ys):
        source = lax.rem(my_y - d + ys, ys)
        for s in range(zs):
            row = lax.rem(my_z - s + zs, zs)
            for k, u_ref in enumerate((uq_ref, uv_ref)):
                rows_ = u_ref.at[block(row, source)]
                remote(
                    rows_,
                    rows_,
                    f_send.at[d - 1, s, k],
                    f_recv.at[d - 1, s, k],
                    my_z * ys + source,
                ).wait_recv()

    square = jnp.float32(0)
    for u_ref in (uq_ref, uv_ref):
        values = u_ref[...].astype(jnp.float32)
        square = square + jnp.sum(values * values)
    sums[0] = jnp.full(sums.shape[1:], square, jnp.float32)
    shared = []
    for d in range(1, t):
        copy = pltpu.make_async_remote_copy(
            src_ref=sums.at[0],
            dst_ref=sums.at[d],
            send_sem=t_send.at[d - 1],
            recv_sem=t_recv.at[d - 1],
            device_id={"tp": lax.rem(col + d, t)},
            device_id_type=pl.DeviceIdType.MESH,
        )
        copy.start()
        shared.append(copy)

    for hop in range(3, n // 2 + 1):
        send_w(hop)

    for copy in shared:
        copy.wait_recv()
    total_ref[...] = jnp.sum(sums[...], axis=0)
    for copy in own:
        copy.wait()
    for copy in started + across + along + gathered + shared:
        copy.wait_send()


def on_device(n, t, inputs, cot_query, cot_value, proj_query, proj_value,
              w_query, w_value, m_query, m_value, v_query, v_value):
    depth = proj_query.shape[0]
    rank = proj_query.shape[1]
    ranks = m_query.shape[0]
    rows = w_query.shape[0]
    width_q = w_query.shape[1]
    width_v = w_value.shape[1]
    tokens = inputs.shape[0]
    tile = 512 if tokens % 512 == 0 else tokens
    half = jnp.bfloat16
    full = jnp.float32
    anywhere = pl.BlockSpec(memory_space=pl.ANY)
    inside = pl.BlockSpec(memory_space=pltpu.VMEM)
    hops = n // 2
    zs = 4 if n % 4 == 0 else n
    ys = n // zs
    gq, gv, uq, uv, lowq, lowv, total = pl.pallas_call(
        functools.partial(kernel, n, t, tile),
        out_shape=(
            jax.ShapeDtypeStruct((depth, width_q), half),
            jax.ShapeDtypeStruct((depth, width_v), half),
            jax.ShapeDtypeStruct((rank, width_q), half),
            jax.ShapeDtypeStruct((rank, width_v), half),
            jax.ShapeDtypeStruct((ranks, width_q), full),
            jax.ShapeDtypeStruct((ranks, width_v), full),
            jax.ShapeDtypeStruct((8, 128), full),
        ),
        in_specs=[anywhere] * 5 + [inside] * 2 + [anywhere] * 4,
        out_specs=(anywhere,) * 2 + (inside,) * 5,
        scratch_shapes=[
            pltpu.VMEM((rank, width_q), full),
            pltpu.VMEM((rank, width_v), full),
            pltpu.VMEM((zs, ys, ranks, width_q), half),
            pltpu.VMEM((zs, ys, ranks, width_v), half),
            pltpu.VMEM((ys, zs, ranks, width_q), half),
            pltpu.VMEM((ys, zs, ranks, width_v), half),
            pltpu.VMEM((zs - 1, ranks, width_q), half),
            pltpu.VMEM((zs - 1, ranks, width_v), half),
            pltpu.VMEM((t, 8, 128), full),
            pltpu.VMEM(proj_query.shape, half),
            pltpu.VMEM(proj_value.shape, half),
            pltpu.VMEM(m_query.shape, full),
            pltpu.VMEM(m_value.shape, full),
            pltpu.VMEM(v_query.shape, full),
            pltpu.VMEM(v_value.shape, full),
            pltpu.SemaphoreType.DMA((6,)),
            pltpu.SemaphoreType.DMA((max(ys - 1, 1), 2)),
            pltpu.SemaphoreType.DMA((max(ys - 1, 1), 2)),
            pltpu.SemaphoreType.DMA((max(ys - 1, 1), zs, 2)),
            pltpu.SemaphoreType.DMA((max(ys - 1, 1), zs, 2)),
            pltpu.SemaphoreType.DMA((2, 2, hops, 2)),
            pltpu.SemaphoreType.DMA((2, 2, hops, 2)),
            pltpu.SemaphoreType.DMA((2,)),
            pltpu.SemaphoreType.DMA((zs - 1, 2)),
            pltpu.SemaphoreType.DMA((zs - 1, 2)),
            pltpu.SemaphoreType.DMA((zs - 1, 2)),
            pltpu.SemaphoreType.DMA((zs - 1, 2)),
            pltpu.SemaphoreType.DMA((t - 1,)),
            pltpu.SemaphoreType.DMA((t - 1,)),
        ],
        compiler_params=pltpu.CompilerParams(
            collective_id=0, has_side_effects=True, vmem_limit_bytes=60 * 2**20
        ),
    )(
        inputs, cot_query, cot_value, proj_query, proj_value,
        w_query.astype(half), w_value.astype(half),
        m_query, m_value, v_query, v_value,
    )
    first_query, second_query = moments(lowq, m_query, v_query)
    first_value, second_value = moments(lowv, m_value, v_value)
    count = rank * t * (width_q + width_v)
    scale = lax.rsqrt(total[0, 0] / count + norm_eps)
    offset = lax.axis_index("fs") * rows
    local_q = lax.dynamic_slice_in_dim(proj_query, offset, rows, 0)
    local_v = lax.dynamic_slice_in_dim(proj_value, offset, rows, 0)

    def dot(a, b):
        return jnp.dot(a, b, preferred_element_type=full)

    def whole(kept, factor, update):
        step = scale * dot(factor, update) + decay_rate * kept.astype(full)
        return (kept.astype(full) - step_rate * step).astype(half)

    step_query = scale * dot(local_q, uq) + decay_rate * w_query
    step_value = scale * dot(local_v, uv) + decay_rate * w_value
    new_query = w_query - step_rate * step_query
    new_value = w_value - step_rate * step_value
    return (
        new_query,
        new_value,
        whole(gq, proj_query, uq),
        whole(gv, proj_value, uv),
        first_query,
        first_value,
        second_query,
        second_value,
        step_query,
        step_value,
    )


def solution(mesh):
    n = mesh.shape["fs"]
    t = mesh.shape["tp"]
    split = P("fs", "tp")
    return jax.shard_map(
        functools.partial(on_device, n, t),
        mesh=mesh,
        in_specs=(P("fs", None), split, split, P(), P()) + (split,) * 6,
        out_specs=(split, split, P(None, "tp"), P(None, "tp")) + (split,) * 6,
        check_vma=False,
    )
```
